32 devices in a mesh: grp: 2 (over y), kv: 4 (over z), tp: 4 (over x, core).
Axes of the slice: x: 2, y: 2, z: 4, core: 2. Of those that a mesh axis runs over, the one named last changes fastest.
Arguments:
- tokens: bfloat16 [32, 4096], P('grp', 'kv'), parts along dimension 0, may hold values from -40 to 40
- lengths: int32 [32], P(('grp', 'kv')), parts along dimension 0, may hold values from 1 to 6, 40 in all
- conv_state_x: bfloat16 [32, 3, 4096], P(('grp', 'kv'), None, 'tp'), parts along dimension 0, may hold values from -6 to 6
- conv_state_bc: bfloat16 [32, 3, 2, 1024], P(('grp', 'kv'), None, None, 'tp'), parts along dimension 0, may hold values from -6 to 6
- ssm_state: float32 [32, 64, 64, 128], P(('grp', 'kv'), 'tp'), parts along dimension 0, may hold values from -0.6 to 0.6
- norm_gain: bfloat16 [4096], P('kv'), may hold values from 0.099609375 to 1.8984375
- w_gate: bfloat16 [4096, 4096], P('kv', 'tp'), may hold values from -0.09375 to 0.09375
- w_value: bfloat16 [4096, 4096], P('kv', 'tp'), may hold values from -0.09375 to 0.09375
- w_key: bfloat16 [4096, 1024], P('kv', 'tp'), may hold values from -0.09375 to 0.09375
- w_query: bfloat16 [4096, 1024], P('kv', 'tp'), may hold values from -0.09375 to 0.09375
- w_step: bfloat16 [4096, 64], P('kv', 'tp'), may hold values from -0.09375 to 0.09375
- step_bias: float32 [64], P('tp'), may hold values from -2 to 0
- decay_log: float32 [64], P('tp'), may hold values from -2 to 1
- conv_x: bfloat16 [4, 4096], P(None, 'tp'), may hold values from -3 to 3
- conv_bc: bfloat16 [4, 2, 1024], P(None, None, 'tp'), may hold values from -3 to 3
- inner_gain: bfloat16 [4096], P('tp'), may hold values from 0.099609375 to 1.8984375
- w_out: bfloat16 [4096, 4096], P('tp', 'kv'), may hold values from -0.09375 to 0.09375
- mlp_gain: bfloat16 [4096], P('kv'), may hold values from 0.099609375 to 1.8984375
- w_up: bfloat16 [4096, 16384], P('kv', 'tp'), may hold values from -0.09375 to 0.09375
- w_down: bfloat16 [16384, 4096], P('tp', 'kv'), may hold values from -0.046875 to 0.046875
Outputs:
- layer_out: bfloat16 [32, 4096], P('grp', 'kv'), parts along dimension 0
- next_state: float32 [32, 64, 64, 128], P(('grp', 'kv'), 'tp'), parts along dimension 0
The draws below stay inside these ranges and needn't reach their ends.
There are 2 independent parts, one for each index of `grp`. The reference program is written for one: setup_inputs(seed, part) draws one part's arguments, and reference() takes and returns one part's arrays. A program takes and returns all parts, laid end to end along the dimension named above; an argument that names none is the same for every part. Nothing has to cross between parts.
All inputs are finite; a program needn't handle non-finite values. No bound on the sum of `lengths` on one device may be relied on, other than what follows from the above.
Results may differ from the reference program's by a relative error of at most 0.008.
Values may be sent and summed in bfloat16 or wider, within the bound.
A program may use at most 64 MiB of HBM per device.

```python
import math
import jax
import jax.numpy as jnp
import numpy as np
from jax import lax

D = 4096
HEADS = 64
HEAD_DIM = 64
GROUPS = 8
STATE = 128
FF = 16384
CONV_WIDTH = 4
INNER = 4096
BATCH = 16


def draw_tokens(key, part):
    base_key = jax.random.fold_in(jax.random.fold_in(key, 11), 0)
    columns = jnp.arange(D, dtype=jnp.float32) / D
    col_scale = 0.6 * jnp.exp(jnp.log(4.0) * columns)[None, :]
    base_draw = jnp.clip(jax.random.normal(base_key, (BATCH, D), jnp.float32), -6.0, 6.0)
    return (base_draw * col_scale).astype(jnp.bfloat16)


def steps_of(stream_key, shape, cuts, smallest, largest):
    factor_of = 1.0
    for position, shards_of in cuts:
        heights = jax.random.uniform(jax.random.fold_in(jax.random.fold_in(stream_key, 6), position), (shards_of,), jnp.float32, smallest / len(cuts), largest / len(cuts))
        factor_of = factor_of * jnp.repeat(jnp.exp(heights), shape[position] // shards_of).reshape((-1,) + (1,) * (len(shape) - 1 - position))
    return factor_of


def profile(number_of, total, reach, slope):
    portions = [(1 << 20) // math.isqrt(standing ** slope) + 1 for standing in range(2, number_of + 1)]
    rest, holding = total - reach - (number_of - 1), [1] * (number_of - 1)
    while rest > 0:
        candidates = [i for i in range(number_of - 1) if holding[i] < reach]
        pool, left = sum([portions[i] for i in candidates]), rest
        for i in candidates:
            addition = min(reach - holding[i], max(1, left * portions[i] // pool), rest)
            holding[i] = holding[i] + addition
            rest = rest - addition
    return np.array([reach] + holding)


def uneven(stream_key, number_of, total, limit, lean):
    if number_of == 2:
        one = jax.random.randint(stream_key, (), max(1, total - limit), min(limit, total - 1) + 1)
        return jnp.stack([one, total - one])
    tallies = jnp.asarray(profile(number_of, total, limit, lean), jnp.int32)
    twos = (number_of - 1) // 2
    source_of, taker = tallies[1:1 + 2 * twos:2], tallies[2:2 + 2 * twos:2]
    room = jnp.minimum(source_of - 1, limit - taker)
    passed = jax.random.randint(jax.random.fold_in(stream_key, 1), (twos,), 0, 1 << 20) % (room + 1)
    tallies = tallies.at[1:1 + 2 * twos:2].set(source_of - passed).at[2:2 + 2 * twos:2].set(taker + passed)
    return tallies[jax.random.permutation(jax.random.fold_in(stream_key, 2), number_of)]


def centred(key, extent, scale, reach, shards=(), held_as=jnp.bfloat16):
    drawn = scale * jax.random.normal(key, extent, jnp.float32)
    if shards:
        drawn = drawn * steps_of(key, extent, shards, -0.22, 0.18)
    return jnp.clip(drawn, -reach, reach).astype(held_as)


def setup_inputs(seed: int = 0, part: int = 0) -> dict:
    key_list = jax.random.split(jax.random.key(seed), 21)
    own_keys = jax.random.split(jax.random.fold_in(key_list[20], part), 21)
    return {
        "tokens": draw_tokens(jax.random.fold_in(jax.random.fold_in(key_list[20], part), 71), part),
        "lengths": uneven(own_keys[1], BATCH, BATCH * 5 // 2, 6, 2).astype(jnp.int32),
        "conv_state_x": centred(own_keys[2], (BATCH, CONV_WIDTH - 1, INNER), 1.0, 6.0, ((0, 4), (2, 4))),
        "conv_state_bc": centred(own_keys[3], (BATCH, CONV_WIDTH - 1, 2, GROUPS * STATE), 1.0, 6.0, ((0, 4), (3, 4))),
        "ssm_state": centred(own_keys[4], (BATCH, HEADS, HEAD_DIM, STATE), 0.1, 0.6, ((0, 4), (1, 4)), jnp.float32),
        "norm_gain": jnp.clip(1.0 + 0.18 * jax.random.normal(key_list[5], (D,), jnp.float32), 0.099609375, 1.8984375).astype(jnp.bfloat16),
        "w_gate": centred(key_list[6], (D, INNER), D ** -0.5, 0.09375, ((0, 4), (1, 4))),
        "w_value": centred(key_list[7], (D, INNER), D ** -0.5, 0.09375, ((0, 4), (1, 4))),
        "w_key": centred(key_list[8], (D, GROUPS * STATE), D ** -0.5, 0.09375, ((0, 4), (1, 4))),
        "w_query": centred(key_list[9], (D, GROUPS * STATE), D ** -0.5, 0.09375, ((0, 4), (1, 4))),
        "w_step": centred(key_list[10], (D, HEADS), D ** -0.5, 0.09375, ((0, 4), (1, 4))),
        "step_bias": jnp.clip(-2.0 + 2.0 * jax.random.uniform(key_list[11], (HEADS,), jnp.float32) ** steps_of(key_list[11], (HEADS,), ((0, 4),), -0.2, 0.2), -2.0, 0.0),
        "decay_log": jnp.clip(-2.0 + 3.0 * jax.random.uniform(key_list[12], (HEADS,), jnp.float32) ** steps_of(key_list[12], (HEADS,), ((0, 4),), -0.2, 0.2), -2.0, 1.0),
        "conv_x": centred(key_list[13], (CONV_WIDTH, INNER), CONV_WIDTH ** -0.5, 3.0, ((1, 4),)),
        "conv_bc": centred(key_list[14], (CONV_WIDTH, 2, GROUPS * STATE), CONV_WIDTH ** -0.5, 3.0, ((2, 4),)),
        "inner_gain": jnp.clip(1.0 + 0.18 * jax.random.normal(key_list[15], (INNER,), jnp.float32), 0.099609375, 1.8984375).astype(jnp.bfloat16),
        "w_out": centred(key_list[16], (INNER, D), INNER ** -0.5, 0.09375, ((0, 4), (1, 4))),
        "mlp_gain": jnp.clip(1.0 + 0.18 * jax.random.normal(key_list[17], (D,), jnp.float32), 0.099609375, 1.8984375).astype(jnp.bfloat16),
        "w_up": centred(key_list[18], (D, FF), D ** -0.5, 0.09375, ((0, 4), (1, 4))),
        "w_down": centred(key_list[19], (FF, D), FF ** -0.5, 0.046875, ((0, 4), (1, 4))),
    }


epsilon = 1e-06

def causal_conv(state_rows, newest, conv_weights):
    extended = jnp.concatenate([state_rows, newest[:, None]], axis=1)
    conv_sum = extended[:, 0] * conv_weights[0].astype(jnp.float32)
    for offset in range(1, conv_weights.shape[0]):
        conv_sum = conv_sum + extended[:, offset] * conv_weights[offset].astype(jnp.float32)
    return jax.nn.silu(conv_sum)

def product(left, right):
    return jnp.dot(left, right, preferred_element_type=jnp.float32)

def reference(tokens, lengths, conv_state_x, conv_state_bc, ssm_state, norm_gain, w_gate, w_value, w_key, w_query, w_step, step_bias, decay_log, conv_x, conv_bc, inner_gain, w_out, mlp_gain, w_up, w_down):
    seq_count = tokens.shape[0]
    per_group = HEADS // GROUPS
    widened = tokens.astype(jnp.float32)
    inverse = lax.rsqrt(lax.optimization_barrier(jnp.mean(widened * widened, axis=1, keepdims=True)) + epsilon)
    scaled = (widened * norm_gain.astype(jnp.float32)).astype(jnp.bfloat16)
    gate_pre = product(scaled, w_gate) * inverse
    value_pre = product(scaled, w_value) * inverse
    key_pre = product(scaled, w_key) * inverse
    query_pre = product(scaled, w_query) * inverse
    step_pre = product(scaled, w_step) * inverse
    row_live = (jnp.arange(CONV_WIDTH - 1, dtype=jnp.int32)[None, :] >= CONV_WIDTH - 1 - lengths[:, None]).astype(jnp.float32)
    live_x = conv_state_x.astype(jnp.float32) * row_live[:, :, None]
    live_bc = conv_state_bc.astype(jnp.float32) * row_live[:, :, None, None]
    mixed_values = causal_conv(live_x, value_pre, conv_x).reshape(seq_count, HEADS, HEAD_DIM)
    key_query = causal_conv(live_bc, jnp.stack([key_pre, query_pre], axis=1), conv_bc)
    key_heads = jnp.repeat(key_query[:, 0].reshape(seq_count, GROUPS, STATE), per_group, axis=1)
    query_heads = jnp.repeat(key_query[:, 1].reshape(seq_count, GROUPS, STATE), per_group, axis=1)
    step_size = jax.nn.softplus(step_pre + step_bias)
    rate_now = -jnp.exp(decay_log) * step_size
    next_state = ssm_state * jnp.exp(rate_now)[:, :, None, None] + (step_size[:, :, None] * mixed_values)[:, :, :, None] * key_heads[:, :, None, :]
    mixer_y = jnp.einsum('bhpn,bhn->bhp', next_state, query_heads, precision=lax.Precision.HIGHEST).reshape(seq_count, INNER)
    gated_rows = mixer_y * jax.nn.silu(gate_pre)
    gated_inverse = lax.rsqrt(lax.optimization_barrier(jnp.mean(gated_rows * gated_rows, axis=1, keepdims=True)) + epsilon)
    gated_low = (gated_rows * inner_gain.astype(jnp.float32)).astype(jnp.bfloat16)
    residual = (widened + product(gated_low, w_out) * gated_inverse).astype(jnp.bfloat16)
    residual_wide = residual.astype(jnp.float32)
    residual_inverse = lax.rsqrt(lax.optimization_barrier(jnp.mean(residual_wide * residual_wide, axis=1, keepdims=True)) + epsilon)
    hidden_low = (residual_wide * mlp_gain.astype(jnp.float32)).astype(jnp.bfloat16)
    activation = jnp.square(jax.nn.relu(product(hidden_low, w_up) * residual_inverse)).astype(jnp.bfloat16)
    layer_out = (residual_wide + product(activation, w_down)).astype(jnp.bfloat16)
    return (layer_out, next_state)
```

```python
import functools

import jax
import jax.numpy as jnp
from jax import lax
from jax.experimental import pallas as pl
from jax.experimental.pallas import tpu as pltpu
from jax.sharding import PartitionSpec as P

D = 4096
HEAD_DIM = 64
STATE = 128
CONV_WIDTH = 4
INNER = 4096
LANES = 128
UP_CHUNKS = 4
TILE = 512

epsilon = 1e-06
F32 = jnp.float32
BF16 = jnp.bfloat16
MESH = pl.DeviceIdType.MESH


def product(left, right):
    return jnp.dot(left, right, preferred_element_type=F32)


def silu(x):
    return x * jax.nn.sigmoid(x)


def tiles(width):
    step = min(TILE, width)
    return [(start, step) for start in range(0, width, step)]


def lane_sum(x):
    return jnp.broadcast_to(jnp.sum(x, axis=1, keepdims=True), (x.shape[0], LANES))


def kernel(
    kv_count,
    tp_count,
    tokens,
    norm_gain,
    mlp_gain,
    inner_gain,
    conv_old,
    conv_tap,
    step_consts,
    ssm_state,
    w_gate,
    w_value,
    w_key,
    w_query,
    w_step,
    w_out,
    w_up,
    w_down,
    layer_out,
    next_state,
    v_gate,
    v_value,
    v_key,
    v_query,
    v_step,
    v_out,
    v_up,
    v_down,
    v_state,
    v_next,
    state_high,
    state_low,
    mix_send,
    mix_recv,
    gate_send,
    gate_recv,
    step_send,
    step_recv,
    low_all,
    low_squares,
    out_all,
    out_squares,
    up_send,
    up_recv,
    up_sq_send,
    up_sq_recv,
    act_all,
    down_all,
    load_sems,
    store_sem,
    kv_send_sems,
    kv_recv_sems,
    tp_send_sems,
    tp_recv_sems,
):
    z = lax.axis_index("kv")
    t = lax.axis_index("tp")
    rows = tokens.shape[0]
    seqs = rows // kv_count
    inner = v_value.shape[1]
    narrow = v_key.shape[1]
    heads = v_step.shape[1]
    group_count = narrow // STATE
    per_group = heads // group_count
    group_width = per_group * HEAD_DIM
    hidden = v_up.shape[1]
    chunk = hidden // UP_CHUNKS

    loads = {}

    def load(name, src, dst):
        copy = pltpu.make_async_copy(src, dst, load_sems.at[len(loads)])
        copy.start()
        loads[name] = copy

    load("value", w_value, v_value)
    load("key", w_key, v_key)
    load("query", w_query, v_query)
    load("step", w_step, v_step)
    load("gate", w_gate, v_gate)
    load("state", ssm_state, v_state)
    load("out", w_out, v_out)

    barrier = pltpu.get_barrier_semaphore()
    for d in range(1, kv_count):
        pl.semaphore_signal(
            barrier, inc=1, device_id={"kv": lax.rem(z + d, kv_count)}, device_id_type=MESH
        )
    for d in range(1, tp_count):
        pl.semaphore_signal(
            barrier, inc=1, device_id={"tp": lax.rem(t + d, tp_count)}, device_id_type=MESH
        )

    started = []

    def exchange(axis, stage, source, target):
        me, count, send_sems, recv_sems = (
            (z, kv_count, kv_send_sems, kv_recv_sems)
            if axis == "kv"
            else (t, tp_count, tp_send_sems, tp_recv_sems)
        )
        copies = []
        for d in range(1, count):
            peer = lax.rem(me + d, count)
            copy = pltpu.make_async_remote_copy(
                src_ref=source(peer),
                dst_ref=target(me),
                send_sem=send_sems.at[stage, d - 1],
                recv_sem=recv_sems.at[stage, d - 1],
                device_id={axis: peer},
                device_id_type=MESH,
            )
            copy.start()
            copies.append(copy)
        started.extend(copies)
        return copies

    def arrive(copies):
        for copy in copies:
            copy.wait_recv()

    def scatter_rows(ref, value, lead=()):
        for j in range(kv_count):
            ref[lead + (j,)] = value[j * seqs : (j + 1) * seqs].astype(ref.dtype)

    def total(ref, count, lead=()):
        acc = ref[lead + (0,)].astype(F32)
        for j in range(1, count):
            acc = acc + ref[lead + (j,)].astype(F32)
        return acc

    def gather_rows(ref, lead=()):
        return jnp.concatenate(
            [ref[lead + (j,)].astype(F32) for j in range(kv_count)], axis=0
        )

    widened = tokens[...].astype(F32)
    scaled = (widened * norm_gain[...].astype(F32)).astype(BF16)
    token_squares = lane_sum(widened * widened)

    def project(weights, send, offset):
        for start, size in tiles(weights.shape[1]):
            piece = product(scaled, weights[:, start : start + size])
            for j in range(kv_count):
                send[j, :, offset + start : offset + start + size] = piece[
                    j * seqs : (j + 1) * seqs
                ].astype(BF16)

    loads["value"].wait()
    project(v_value, mix_send, 0)
    loads["key"].wait()
    project(v_key, mix_send, inner)
    loads["query"].wait()
    project(v_query, mix_send, inner + narrow)
    loads["step"].wait()
    step_part = product(scaled, v_step[...])
    step_part = jnp.concatenate(
        [step_part, jnp.zeros((rows, LANES - heads), F32), token_squares], axis=1
    )
    scatter_rows(step_send, step_part)
    pl.semaphore_wait(barrier, kv_count + tp_count - 2)
    step_copies = exchange("kv", 0, lambda p: step_send.at[p], lambda m: step_recv.at[m])
    mix_copies = exchange("kv", 1, lambda p: mix_send.at[p], lambda m: mix_recv.at[m])
    loads["gate"].wait()
    for c in range(UP_CHUNKS):
        load(
            f"up{c}",
            w_up.at[:, c * chunk : (c + 1) * chunk],
            v_up.at[:, c * chunk : (c + 1) * chunk],
        )
    for c in range(UP_CHUNKS):
        load(
            f"down{c}",
            w_down.at[c * chunk : (c + 1) * chunk],
            v_down.at[c * chunk : (c + 1) * chunk],
        )
    project(v_gate, gate_send, 0)
    gate_copies = exchange("kv", 2, lambda p: gate_send.at[p], lambda m: gate_recv.at[m])
    step_recv[z] = step_send[z]
    mix_recv[z] = mix_send[z]
    gate_recv[z] = gate_send[z]

    loads["state"].wait()
    for b in range(seqs):
        state = v_state[b]
        high = state.astype(BF16)
        state_high[b] = high
        state_low[b] = (state - high.astype(F32)).astype(BF16)

    arrive(step_copies)
    steps = total(step_recv, kv_count)
    inverse = lax.rsqrt(steps[:, LANES : LANES + 1] / D + epsilon)
    step_size = jax.nn.softplus(steps[:, :LANES] * inverse + step_consts[0:1])
    decay = jnp.exp(-jnp.exp(step_consts[1:2]) * step_size)
    head_of = lax.broadcasted_iota(jnp.int32, (LANES, inner), 1) // HEAD_DIM
    one_hot = jnp.where(
        head_of == lax.broadcasted_iota(jnp.int32, (LANES, inner), 0), 1.0, 0.0
    ).astype(F32)
    spread = jnp.dot(
        jnp.concatenate([step_size, decay], axis=0),
        one_hot,
        precision=lax.Precision.HIGHEST,
        preferred_element_type=F32,
    )
    step_wide, decay_wide = spread[:seqs], spread[seqs:]
    arrive(mix_copies)
    mixed = silu(conv_old[...] + total(mix_recv, kv_count) * inverse * conv_tap[...])
    input_wide = step_wide * mixed[:, :inner]
    keys = mixed[:, inner : inner + narrow]
    queries = mixed[:, inner + narrow :]

    pieces = []
    for g in range(group_count):
        query = queries[:, g * STATE : (g + 1) * STATE]
        key = keys[:, g * STATE : (g + 1) * STATE]
        query_high = query.astype(BF16).astype(F32)
        both = jnp.concatenate([query_high, query - query_high], axis=0).astype(BF16)
        lines = []
        for b in range(seqs):
            span = slice(g * per_group, (g + 1) * per_group)
            high = state_high[b, span].reshape(group_width, STATE)
            low = state_low[b, span].reshape(group_width, STATE)
            dims = (((1,), (1,)), ((), ()))
            with_high = lax.dot_general(both, high, dims, preferred_element_type=F32)
            with_low = lax.dot_general(both, low, dims, preferred_element_type=F32)
            lines.append(
                with_high[b : b + 1] + with_high[seqs + b : seqs + b + 1] + with_low[b : b + 1]
            )
        from_state = jnp.concatenate(lines, axis=0)
        overlap = jnp.sum(key * query, axis=1, keepdims=True)
        columns = slice(g * group_width, (g + 1) * group_width)
        pieces.append(decay_wide[:, columns] * from_state + input_wide[:, columns] * overlap)
    mixer_y = jnp.concatenate(pieces, axis=1)
    arrive(gate_copies)
    gated = mixer_y * silu(total(gate_recv, kv_count) * inverse)
    low_all[z] = (gated * inner_gain[...].astype(F32)).astype(BF16)
    low_squares[z] = lane_sum(gated * gated)
    low_copies = exchange("kv", 3, lambda p: low_all.at[z], lambda m: low_all.at[m])
    sq_copies = exchange("kv", 4, lambda p: low_squares.at[z], lambda m: low_squares.at[m])

    padded = jnp.concatenate(
        [input_wide, jnp.zeros((LANES - seqs, inner), F32)], axis=0
    )
    upright = jnp.transpose(padded)
    for b in range(seqs):
        for h in range(heads):
            g = h // per_group
            v_next[b, h] = (
                v_state[b, h] * decay[b : b + 1, h : h + 1]
                + upright[h * HEAD_DIM : (h + 1) * HEAD_DIM, b : b + 1]
                * keys[b : b + 1, g * STATE : (g + 1) * STATE]
            )
    store = pltpu.make_async_copy(v_next, next_state, store_sem)
    store.start()

    loads["out"].wait()
    arrive(low_copies)
    lows = gather_rows(low_all).astype(BF16)
    for start, size in tiles(v_out.shape[1]):
        out_all[t, :, start : start + size] = product(
            lows, v_out[:, start : start + size]
        ).astype(BF16)
    arrive(sq_copies)
    out_squares[t] = gather_rows(low_squares)
    out_copies = exchange("tp", 0, lambda p: out_all.at[t], lambda m: out_all.at[m])
    out_sq_copies = exchange("tp", 1, lambda p: out_squares.at[t], lambda m: out_squares.at[m])
    arrive(out_sq_copies)
    out_inverse = lax.rsqrt(total(out_squares, tp_count)[:, :1] / INNER + epsilon)
    arrive(out_copies)
    residual = (widened + total(out_all, tp_count) * out_inverse).astype(BF16).astype(F32)
    hidden_low = (residual * mlp_gain[...].astype(F32)).astype(BF16)
    scatter_rows(up_sq_send, lane_sum(residual * residual))
    up_sq_copies = exchange("kv", 5, lambda p: up_sq_send.at[p], lambda m: up_sq_recv.at[m])

    up_copies = []
    for c in range(UP_CHUNKS):
        loads[f"up{c}"].wait()
        for start, size in tiles(chunk):
            base = c * chunk + start
            piece = product(hidden_low, v_up[:, base : base + size])
            for j in range(kv_count):
                up_send[c, j, :, start : start + size] = piece[
                    j * seqs : (j + 1) * seqs
                ].astype(BF16)
        up_copies.append(
            exchange(
                "kv",
                6 + c,
                lambda p, c=c: up_send.at[c, p],
                lambda m, c=c: up_recv.at[c, m],
            )
        )
        up_recv[c, z] = up_send[c, z]
    up_sq_recv[z] = up_sq_send[z]
    arrive(up_sq_copies)
    up_inverse = lax.rsqrt(total(up_sq_recv, kv_count)[:, :1] / D + epsilon)
    act_copies = []
    for c in range(UP_CHUNKS):
        arrive(up_copies[c])
        active = jnp.maximum(total(up_recv, kv_count, (c,)) * up_inverse, 0.0)
        act_all[c, z] = (active * active).astype(BF16)
        act_copies.append(
            exchange(
                "kv",
                6 + UP_CHUNKS + c,
                lambda p, c=c: act_all.at[c, z],
                lambda m, c=c: act_all.at[c, m],
            )
        )
    down = jnp.zeros((rows, v_down.shape[1]), F32)
    for c in range(UP_CHUNKS):
        loads[f"down{c}"].wait()
        arrive(act_copies[c])
        acts = gather_rows(act_all, (c,)).astype(BF16)
        down = down + product(acts, v_down[c * chunk : (c + 1) * chunk])
    down_all[t] = down.astype(BF16)
    down_copies = exchange("tp", 2, lambda p: down_all.at[t], lambda m: down_all.at[m])
    arrive(down_copies)
    layer_out[...] = (residual + total(down_all, tp_count)).astype(BF16)
    for copy in started:
        copy.wait_send()
    store.wait()


def per_device(
    kv_count,
    tp_count,
    tokens,
    lengths,
    conv_state_x,
    conv_state_bc,
    ssm_state,
    norm_gain,
    w_gate,
    w_value,
    w_key,
    w_query,
    w_step,
    step_bias,
    decay_log,
    conv_x,
    conv_bc,
    inner_gain,
    w_out,
    mlp_gain,
    w_up,
    w_down,
):
    rows, depth = tokens.shape
    seqs = lengths.shape[0]
    inner, narrow, heads = w_value.shape[1], w_key.shape[1], w_step.shape[1]
    hidden = w_up.shape[1]
    chunk = hidden // UP_CHUNKS
    row_live = (
        jnp.arange(CONV_WIDTH - 1, dtype=jnp.int32)[None, :] >= CONV_WIDTH - 1 - lengths[:, None]
    ).astype(F32)
    taps = jnp.concatenate([conv_x, conv_bc.reshape(CONV_WIDTH, 2 * narrow)], axis=1).astype(F32)
    held = jnp.concatenate(
        [conv_state_x, conv_state_bc.reshape(seqs, CONV_WIDTH - 1, 2 * narrow)], axis=2
    ).astype(F32)
    conv_old = jnp.zeros((seqs, inner + 2 * narrow), F32)
    for k in range(CONV_WIDTH - 1):
        conv_old = conv_old + held[:, k] * row_live[:, k][:, None] * taps[k]
    conv_tap = taps[CONV_WIDTH - 1 :]
    step_consts = jnp.pad(jnp.stack([step_bias, decay_log]), ((0, 0), (0, LANES - heads)))

    vmem = pl.BlockSpec(memory_space=pltpu.VMEM)
    hbm = pl.BlockSpec(memory_space=pl.ANY)
    mixed = inner + 2 * narrow
    width = w_out.shape[1]
    stages = 6 + 2 * UP_CHUNKS
    return pl.pallas_call(
        functools.partial(kernel, kv_count, tp_count),
        out_shape=(
            jax.ShapeDtypeStruct((rows, width), BF16),
            jax.ShapeDtypeStruct(ssm_state.shape, F32),
        ),
        in_specs=[vmem] * 7 + [hbm] * 9,
        out_specs=(vmem, hbm),
        scratch_shapes=[
            pltpu.VMEM(w_gate.shape, BF16),
            pltpu.VMEM(w_value.shape, BF16),
            pltpu.VMEM(w_key.shape, BF16),
            pltpu.VMEM(w_query.shape, BF16),
            pltpu.VMEM(w_step.shape, BF16),
            pltpu.VMEM(w_out.shape, BF16),
            pltpu.VMEM(w_up.shape, BF16),
            pltpu.VMEM(w_down.shape, BF16),
            pltpu.VMEM(ssm_state.shape, F32),
            pltpu.VMEM(ssm_state.shape, F32),
            pltpu.VMEM(ssm_state.shape, BF16),
            pltpu.VMEM(ssm_state.shape, BF16),
            pltpu.VMEM((kv_count, seqs, mixed), BF16),
            pltpu.VMEM((kv_count, seqs, mixed), BF16),
            pltpu.VMEM((kv_count, seqs, inner), BF16),
            pltpu.VMEM((kv_count, seqs, inner), BF16),
            pltpu.VMEM((kv_count, seqs, 2 * LANES), F32),
            pltpu.VMEM((kv_count, seqs, 2 * LANES), F32),
            pltpu.VMEM((kv_count, seqs, inner), BF16),
            pltpu.VMEM((kv_count, seqs, LANES), F32),
            pltpu.VMEM((tp_count, rows, width), BF16),
            pltpu.VMEM((tp_count, rows, LANES), F32),
            pltpu.VMEM((UP_CHUNKS, kv_count, seqs, chunk), BF16),
            pltpu.VMEM((UP_CHUNKS, kv_count, seqs, chunk), BF16),
            pltpu.VMEM((kv_count, seqs, LANES), F32),
            pltpu.VMEM((kv_count, seqs, LANES), F32),
            pltpu.VMEM((UP_CHUNKS, kv_count, seqs, chunk), BF16),
            pltpu.VMEM((tp_count, rows, width), BF16),
            pltpu.SemaphoreType.DMA((7 + 2 * UP_CHUNKS,)),
            pltpu.SemaphoreType.DMA,
            pltpu.SemaphoreType.DMA((stages, max(kv_count - 1, 1))),
            pltpu.SemaphoreType.DMA((stages, max(kv_count - 1, 1))),
            pltpu.SemaphoreType.DMA((3, max(tp_count - 1, 1))),
            pltpu.SemaphoreType.DMA((3, max(tp_count - 1, 1))),
        ],
        compiler_params=pltpu.CompilerParams(
            collective_id=0, has_side_effects=True, vmem_limit_bytes=60 * 1024 * 1024
        ),
    )(
        tokens,
        norm_gain[None],
        mlp_gain[None],
        inner_gain[None],
        conv_old,
        conv_tap,
        step_consts,
        ssm_state,
        w_gate,
        w_value,
        w_key,
        w_query,
        w_step,
        w_out,
        w_up,
        w_down,
    )


def solution(mesh):
    return jax.shard_map(
        functools.partial(per_device, mesh.shape["kv"], mesh.shape["tp"]),
        mesh=mesh,
        in_specs=(
            P("grp", "kv"),
            P(("grp", "kv")),
            P(("grp", "kv"), None, "tp"),
            P(("grp", "kv"), None, None, "tp"),
            P(("grp", "kv"), "tp", None, None),
            P("kv"),
            P("kv", "tp"),
            P("kv", "tp"),
            P("kv", "tp"),
            P("kv", "tp"),
            P("kv", "tp"),
            P("tp"),
            P("tp"),
            P(None, "tp"),
            P(None, None, "tp"),
            P("tp"),
            P("tp", "kv"),
            P("kv"),
            P("kv", "tp"),
            P("tp", "kv"),
        ),
        out_specs=(P("grp", "kv"), P(("grp", "kv"), "tp", None, None)),
        check_vma=False,
    )
```

```python
import functools

import jax
import jax.numpy as jnp
from jax import lax
from jax.experimental import pallas as pl
from jax.experimental.pallas import tpu as pltpu
from jax.sharding import PartitionSpec as P

D = 4096
HEAD_DIM = 64
STATE = 128
CONV_WIDTH = 4
INNER = 4096
LANES = 128
VMEM_BYTES = 67043328
UP_CHUNKS = 4
TILE = 512

epsilon = 1e-06
F32 = jnp.float32
BF16 = jnp.bfloat16
MESH = pl.DeviceIdType.MESH


def product(left, right):
    return jnp.dot(left, right, preferred_element_type=F32)


def silu(x):
    return x * jax.nn.sigmoid(x)


def tiles(width):
    step = min(TILE, width)
    return [(start, step) for start in range(0, width, step)]


def lane_sum(x):
    return jnp.broadcast_to(jnp.sum(x, axis=1, keepdims=True), (x.shape[0], LANES))


def kernel(
    kv_count,
    tp_count,
    h_tokens,
    h_lengths,
    h_conv_state_x,
    h_conv_state_bc,
    h_norm_gain,
    h_mlp_gain,
    h_inner_gain,
    h_step_bias,
    h_decay_log,
    h_conv_x,
    h_conv_bc,
    ssm_state,
    w_gate,
    w_value,
    w_key,
    w_query,
    w_step,
    w_out,
    w_up,
    w_down,
    layer_out,
    next_state,
    v_gate,
    v_value,
    v_key,
    v_query,
    v_step,
    v_out,
    v_up,
    v_down,
    v_state,
    state_high,
    state_low,
    tokens,
    lengths,
    conv_state_x,
    conv_state_bc,
    norm_gain,
    mlp_gain,
    inner_gain,
    step_bias,
    decay_log,
    conv_x,
    conv_bc,
    mix_send,
    mix_recv,
    gate_send,
    gate_recv,
    step_send,
    step_recv,
    low_all,
    low_squares,
    out_all,
    out_squares,
    up_send,
    up_recv,
    up_sq_send,
    up_sq_recv,
    act_all,
    down_all,
    load_sems,
    kv_send_sems,
    kv_recv_sems,
    tp_send_sems,
    tp_recv_sems,
):
    z = lax.axis_index("kv")
    t = lax.axis_index("tp")
    rows = tokens.shape[0]
    seqs = rows // kv_count
    inner = v_value.shape[1]
    narrow = v_key.shape[1]
    heads = v_step.shape[0]
    group_count = narrow // STATE
    per_group = heads // group_count
    group_width = per_group * HEAD_DIM
    hidden = v_up.shape[1]
    chunk = hidden // UP_CHUNKS

    loads = {}

    def load(name, src, dst):
        copy = pltpu.make_async_copy(src, dst, load_sems.at[len(loads)])
        copy.start()
        loads[name] = copy

    load("tokens", h_tokens, tokens)
    load("norm_gain", h_norm_gain, norm_gain)
    load("value", w_value, v_value)
    load("key", w_key, v_key)
    load("query", w_query, v_query)
    load("step", w_step, v_step)
    load("gate", w_gate, v_gate)
    small = [
        ("lengths", h_lengths, lengths),
        ("conv_state_x", h_conv_state_x, conv_state_x),
        ("conv_state_bc", h_conv_state_bc, conv_state_bc),
        ("mlp_gain", h_mlp_gain, mlp_gain),
        ("inner_gain", h_inner_gain, inner_gain),
        ("step_bias", h_step_bias, step_bias),
        ("decay_log", h_decay_log, decay_log),
        ("conv_x", h_conv_x, conv_x),
        ("conv_bc", h_conv_bc, conv_bc),
    ]
    for item in small:
        load(*item)
    load("state", ssm_state, v_state)
    load("out", w_out, v_out)

    barrier = pltpu.get_barrier_semaphore()
    for d in range(1, kv_count):
        pl.semaphore_signal(
            barrier, inc=1, device_id={"kv": lax.rem(z + d, kv_count)}, device_id_type=MESH
        )
    for d in range(1, tp_count):
        pl.semaphore_signal(
            barrier, inc=1, device_id={"tp": lax.rem(t + d, tp_count)}, device_id_type=MESH
        )

    started = []

    def exchange(axis, stage, source, target):
        me, count, send_sems, recv_sems = (
            (z, kv_count, kv_send_sems, kv_recv_sems)
            if axis == "kv"
            else (t, tp_count, tp_send_sems, tp_recv_sems)
        )
        copies = []
        for d in range(1, count):
            peer = lax.rem(me + d, count)
            copy = pltpu.make_async_remote_copy(
                src_ref=source(peer),
                dst_ref=target(me),
                send_sem=send_sems.at[stage, d - 1],
                recv_sem=recv_sems.at[stage, d - 1],
                device_id={axis: peer},
                device_id_type=MESH,
            )
            copy.start()
            copies.append(copy)
        started.extend(copies)
        return copies

    def arrive(copies):
        for copy in copies:
            copy.wait_recv()

    def scatter_rows(ref, value, lead=()):
        for j in range(kv_count):
            ref[lead + (j,)] = value[j * seqs : (j + 1) * seqs].astype(ref.dtype)

    def total(ref, count, lead=()):
        acc = ref[lead + (0,)].astype(F32)
        for j in range(1, count):
            acc = acc + ref[lead + (j,)].astype(F32)
        return acc

    def gather_rows(ref, lead=()):
        return jnp.concatenate(
            [ref[lead + (j,)].astype(F32) for j in range(kv_count)], axis=0
        )

    def gain(ref):
        return ref[...].astype(F32).reshape(1, ref.shape[0])

    loads["tokens"].wait()
    loads["norm_gain"].wait()
    widened = tokens[...].astype(F32)
    scaled = (widened * gain(norm_gain)).astype(BF16)
    token_squares = lane_sum(widened * widened)

    def project(weights, send, offset):
        for start, size in tiles(weights.shape[1]):
            piece = product(scaled, weights[:, start : start + size])
            for j in range(kv_count):
                send[j, :, offset + start : offset + start + size] = piece[
                    j * seqs : (j + 1) * seqs
                ].astype(BF16)

    loads["value"].wait()
    project(v_value, mix_send, 0)
    loads["key"].wait()
    project(v_key, mix_send, inner)
    loads["query"].wait()
    project(v_query, mix_send, inner + narrow)
    loads["step"].wait()
    step_part = lax.dot_general(
        scaled, v_step[...], (((1,), (1,)), ((), ())), preferred_element_type=F32
    )
    step_part = jnp.concatenate(
        [step_part, jnp.zeros((rows, LANES - heads), F32), token_squares], axis=1
    )
    scatter_rows(step_send, step_part)
    pl.semaphore_wait(barrier, kv_count + tp_count - 2)
    step_copies = exchange("kv", 0, lambda p: step_send.at[p], lambda m: step_recv.at[m])
    mix_copies = exchange("kv", 1, lambda p: mix_send.at[p], lambda m: mix_recv.at[m])
    loads["gate"].wait()
    for c in range(UP_CHUNKS):
        load(
            f"up{c}",
            w_up.at[:, c * chunk : (c + 1) * chunk],
            v_up.at[:, c * chunk : (c + 1) * chunk],
        )
    for c in range(UP_CHUNKS):
        load(
            f"down{c}",
            w_down.at[c * chunk : (c + 1) * chunk],
            v_down.at[c * chunk : (c + 1) * chunk],
        )
    project(v_gate, gate_send, 0)
    gate_copies = exchange("kv", 2, lambda p: gate_send.at[p], lambda m: gate_recv.at[m])
    step_recv[z] = step_send[z]
    mix_recv[z] = mix_send[z]
    gate_recv[z] = gate_send[z]

    loads["state"].wait()
    for b in range(seqs):
        state = v_state[b]
        high = state.astype(BF16)
        state_high[b] = high
        state_low[b] = (state - high.astype(F32)).astype(BF16)

    for name, _, _ in small:
        loads[name].wait()
    seq_of = lax.broadcasted_iota(jnp.int32, (seqs, 1), 0)
    seen = jnp.zeros((seqs, 1), jnp.int32)
    for b in range(seqs):
        seen = jnp.where(seq_of == b, lengths[b], seen)
    lane_of = lax.broadcasted_iota(jnp.int32, (1, LANES), 1)
    bias_row = jnp.zeros((1, LANES), F32)
    log_row = jnp.zeros((1, LANES), F32)
    for h in range(heads):
        bias_row = jnp.where(lane_of == h, step_bias[h], bias_row)
        log_row = jnp.where(lane_of == h, decay_log[h], log_row)

    taps = jnp.concatenate(
        [conv_x[...].astype(F32)] + [conv_bc[:, i].astype(F32) for i in range(2)], axis=1
    )
    conv_old = jnp.zeros((seqs, inner + 2 * narrow), F32)
    for k in range(CONV_WIDTH - 1):
        held = jnp.concatenate(
            [conv_state_x[k].astype(F32)]
            + [conv_state_bc[:, k, i].astype(F32) for i in range(2)],
            axis=1,
        )
        live = jnp.where(seen >= CONV_WIDTH - 1 - k, 1.0, 0.0)
        conv_old = conv_old + held * live * taps[k : k + 1]
    conv_tap = taps[CONV_WIDTH - 1 :]

    arrive(step_copies)
    steps = total(step_recv, kv_count)
    inverse = lax.rsqrt(steps[:, LANES : LANES + 1] / D + epsilon)
    step_size = jax.nn.softplus(steps[:, :LANES] * inverse + bias_row)
    decay = jnp.exp(-jnp.exp(log_row) * step_size)
    head_of = lax.broadcasted_iota(jnp.int32, (LANES, inner), 1) // HEAD_DIM
    one_hot = jnp.where(
        head_of == lax.broadcasted_iota(jnp.int32, (LANES, inner), 0), 1.0, 0.0
    ).astype(F32)
    spread = jnp.dot(
        jnp.concatenate([step_size, decay], axis=0),
        one_hot,
        precision=lax.Precision.HIGHEST,
        preferred_element_type=F32,
    )
    step_wide, decay_wide = spread[:seqs], spread[seqs:]
    arrive(mix_copies)
    mixed = silu(conv_old + total(mix_recv, kv_count) * inverse * conv_tap)
    input_wide = step_wide * mixed[:, :inner]
    keys = mixed[:, inner : inner + narrow]
    queries = mixed[:, inner + narrow :]

    pieces = []
    for g in range(group_count):
        query = queries[:, g * STATE : (g + 1) * STATE]
        key = keys[:, g * STATE : (g + 1) * STATE]
        query_high = query.astype(BF16).astype(F32)
        both = jnp.concatenate([query_high, query - query_high], axis=0).astype(BF16)
        lines = []
        for b in range(seqs):
            span = slice(g * per_group, (g + 1) * per_group)
            high = state_high[b, span].reshape(group_width, STATE)
            low = state_low[b, span].reshape(group_width, STATE)
            dims = (((1,), (1,)), ((), ()))
            with_high = lax.dot_general(both, high, dims, preferred_element_type=F32)
            with_low = lax.dot_general(both, low, dims, preferred_element_type=F32)
            lines.append(
                with_high[b : b + 1] + with_high[seqs + b : seqs + b + 1] + with_low[b : b + 1]
            )
        from_state = jnp.concatenate(lines, axis=0)
        overlap = jnp.sum(key * query, axis=1, keepdims=True)
        columns = slice(g * group_width, (g + 1) * group_width)
        pieces.append(decay_wide[:, columns] * from_state + input_wide[:, columns] * overlap)
    mixer_y = jnp.concatenate(pieces, axis=1)
    arrive(gate_copies)
    gated = mixer_y * silu(total(gate_recv, kv_count) * inverse)
    low_all[z] = (gated * gain(inner_gain)).astype(BF16)
    low_squares[z] = lane_sum(gated * gated)
    low_copies = exchange("kv", 3, lambda p: low_all.at[z], lambda m: low_all.at[m])
    sq_copies = exchange("kv", 4, lambda p: low_squares.at[z], lambda m: low_squares.at[m])

    padded = jnp.concatenate(
        [input_wide, jnp.zeros((LANES - seqs, inner), F32)], axis=0
    )
    upright = jnp.transpose(padded)
    for b in range(seqs):
        for h in range(heads):
            g = h // per_group
            next_state[b, h] = (
                v_state[b, h] * decay[b : b + 1, h : h + 1]
                + upright[h * HEAD_DIM : (h + 1) * HEAD_DIM, b : b + 1]
                * keys[b : b + 1, g * STATE : (g + 1) * STATE]
            )

    loads["out"].wait()
    arrive(low_copies)
    lows = gather_rows(low_all).astype(BF16)
    for start, size in tiles(v_out.shape[1]):
        out_all[t, :, start : start + size] = product(
            lows, v_out[:, start : start + size]
        ).astype(BF16)
    arrive(sq_copies)
    out_squares[t] = gather_rows(low_squares)
    out_copies = exchange("tp", 0, lambda p: out_all.at[t], lambda m: out_all.at[m])
    out_sq_copies = exchange("tp", 1, lambda p: out_squares.at[t], lambda m: out_squares.at[m])
    arrive(out_sq_copies)
    out_inverse = lax.rsqrt(total(out_squares, tp_count)[:, :1] / INNER + epsilon)
    arrive(out_copies)
    residual = (widened + total(out_all, tp_count) * out_inverse).astype(BF16).astype(F32)
    hidden_low = (residual * gain(mlp_gain)).astype(BF16)
    scatter_rows(up_sq_send, lane_sum(residual * residual))
    up_sq_copies = exchange("kv", 5, lambda p: up_sq_send.at[p], lambda m: up_sq_recv.at[m])

    up_copies = []
    for c in range(UP_CHUNKS):
        loads[f"up{c}"].wait()
        for start, size in tiles(chunk):
            base = c * chunk + start
            piece = product(hidden_low, v_up[:, base : base + size])
            for j in range(kv_count):
                up_send[c, j, :, start : start + size] = piece[
                    j * seqs : (j + 1) * seqs
                ].astype(BF16)
        up_copies.append(
            exchange(
                "kv",
                6 + c,
                lambda p, c=c: up_send.at[c, p],
                lambda m, c=c: up_recv.at[c, m],
            )
        )
        up_recv[c, z] = up_send[c, z]
    up_sq_recv[z] = up_sq_send[z]
    arrive(up_sq_copies)
    up_inverse = lax.rsqrt(total(up_sq_recv, kv_count)[:, :1] / D + epsilon)
    act_copies = []
    for c in range(UP_CHUNKS):
        arrive(up_copies[c])
        active = jnp.maximum(total(up_recv, kv_count, (c,)) * up_inverse, 0.0)
        act_all[c, z] = (active * active).astype(BF16)
        act_copies.append(
            exchange(
                "kv",
                6 + UP_CHUNKS + c,
                lambda p, c=c: act_all.at[c, z],
                lambda m, c=c: act_all.at[c, m],
            )
        )
    down = jnp.zeros((rows, v_down.shape[1]), F32)
    for c in range(UP_CHUNKS):
        loads[f"down{c}"].wait()
        arrive(act_copies[c])
        acts = gather_rows(act_all, (c,)).astype(BF16)
        down = down + product(acts, v_down[c * chunk : (c + 1) * chunk])
    down_all[t] = down.astype(BF16)
    down_copies = exchange("tp", 2, lambda p: down_all.at[t], lambda m: down_all.at[m])
    arrive(down_copies)
    layer_out[...] = (residual + total(down_all, tp_count)).astype(BF16)
    for copy in started:
        copy.wait_send()


def per_device(
    kv_count,
    tp_count,
    tokens,
    lengths,
    conv_state_x,
    conv_state_bc,
    ssm_state,
    norm_gain,
    w_gate,
    w_value,
    w_key,
    w_query,
    w_step,
    step_bias,
    decay_log,
    conv_x,
    conv_bc,
    inner_gain,
    w_out,
    mlp_gain,
    w_up,
    w_down,
):
    rows, depth = tokens.shape
    seqs = lengths.shape[0]
    inner, narrow, heads = w_value.shape[1], w_key.shape[1], w_step.shape[1]
    hidden = w_up.shape[1]
    chunk = hidden // UP_CHUNKS
    results = 4 * ssm_state.size + 2 * rows * w_out.shape[1]
    grant = (VMEM_BYTES - results) // 4096 * 4096 - 4096
    vmem = pl.BlockSpec(memory_space=pltpu.VMEM)
    hbm = pl.BlockSpec(memory_space=pltpu.HBM)
    mixed = inner + 2 * narrow
    width = w_out.shape[1]
    stages = 6 + 2 * UP_CHUNKS
    return pl.pallas_call(
        functools.partial(kernel, kv_count, tp_count),
        out_shape=(
            pltpu.VMEM((rows, width), BF16),
            pltpu.VMEM(ssm_state.shape, F32),
        ),
        in_specs=[hbm] * 20,
        out_specs=(vmem, vmem),
        scratch_shapes=[
            pltpu.VMEM(w_gate.shape, BF16),
            pltpu.VMEM(w_value.shape, BF16),
            pltpu.VMEM(w_key.shape, BF16),
            pltpu.VMEM(w_query.shape, BF16),
            pltpu.VMEM(w_step.shape[::-1], BF16),
            pltpu.VMEM(w_out.shape, BF16),
            pltpu.VMEM(w_up.shape, BF16),
            pltpu.VMEM(w_down.shape, BF16),
            pltpu.VMEM(ssm_state.shape, F32),
            pltpu.VMEM(ssm_state.shape, BF16),
            pltpu.VMEM(ssm_state.shape, BF16),
            pltpu.VMEM(tokens.shape, BF16),
            pltpu.SMEM(lengths.shape, jnp.int32),
            pltpu.VMEM((CONV_WIDTH - 1, seqs, inner), BF16),
            pltpu.VMEM(conv_state_bc.shape, BF16),
            pltpu.VMEM(norm_gain.shape, BF16),
            pltpu.VMEM(mlp_gain.shape, BF16),
            pltpu.VMEM(inner_gain.shape, BF16),
            pltpu.SMEM(step_bias.shape, F32),
            pltpu.SMEM(decay_log.shape, F32),
            pltpu.VMEM(conv_x.shape, BF16),
            pltpu.VMEM(conv_bc.shape, BF16),
            pltpu.VMEM((kv_count, seqs, mixed), BF16),
            pltpu.VMEM((kv_count, seqs, mixed), BF16),
            pltpu.VMEM((kv_count, seqs, inner), BF16),
            pltpu.VMEM((kv_count, seqs, inner), BF16),
            pltpu.VMEM((kv_count, seqs, 2 * LANES), F32),
            pltpu.VMEM((kv_count, seqs, 2 * LANES), F32),
            pltpu.VMEM((kv_count, seqs, inner), BF16),
            pltpu.VMEM((kv_count, seqs, LANES), F32),
            pltpu.VMEM((tp_count, rows, width), BF16),
            pltpu.VMEM((tp_count, rows, LANES), F32),
            pltpu.VMEM((UP_CHUNKS, kv_count, seqs, chunk), BF16),
            pltpu.VMEM((UP_CHUNKS, kv_count, seqs, chunk), BF16),
            pltpu.VMEM((kv_count, seqs, LANES), F32),
            pltpu.VMEM((kv_count, seqs, LANES), F32),
            pltpu.VMEM((UP_CHUNKS, kv_count, seqs, chunk), BF16),
            pltpu.VMEM((tp_count, rows, width), BF16),
            pltpu.SemaphoreType.DMA((18 + 2 * UP_CHUNKS,)),
            pltpu.SemaphoreType.DMA((stages, max(kv_count - 1, 1))),
            pltpu.SemaphoreType.DMA((stages, max(kv_count - 1, 1))),
            pltpu.SemaphoreType.DMA((3, max(tp_count - 1, 1))),
            pltpu.SemaphoreType.DMA((3, max(tp_count - 1, 1))),
        ],
        compiler_params=pltpu.CompilerParams(
            collective_id=0, has_side_effects=True, vmem_limit_bytes=grant
        ),
    )(
        tokens,
        lengths,
        jnp.swapaxes(conv_state_x, 0, 1),
        conv_state_bc,
        norm_gain,
        mlp_gain,
        inner_gain,
        step_bias,
        decay_log,
        conv_x,
        conv_bc,
        ssm_state,
        w_gate,
        w_value,
        w_key,
        w_query,
        w_step.T,
        w_out,
        w_up,
        w_down,
    )


def solution(mesh):
    return jax.shard_map(
        functools.partial(per_device, mesh.shape["kv"], mesh.shape["tp"]),
        mesh=mesh,
        in_specs=(
            P("grp", "kv"),
            P(("grp", "kv")),
            P(("grp", "kv"), None, "tp"),
            P(("grp", "kv"), None, None, "tp"),
            P(("grp", "kv"), "tp", None, None),
            P("kv"),
            P("kv", "tp"),
            P("kv", "tp"),
            P("kv", "tp"),
            P("kv", "tp"),
            P("kv", "tp"),
            P("tp"),
            P("tp"),
            P(None, "tp"),
            P(None, None, "tp"),
            P("tp"),
            P("tp", "kv"),
            P("kv"),
            P("kv", "tp"),
            P("tp", "kv"),
        ),
        out_specs=(P("grp", "kv"), P(("grp", "kv"), "tp", None, None)),
        check_vma=False,
    )
```

```python
import functools

import jax
import jax.numpy as jnp
from jax import lax
from jax.experimental import pallas as pl
from jax.experimental.pallas import tpu as pltpu
from jax.sharding import PartitionSpec as P

D = 4096
HEAD_DIM = 64
STATE = 128
CONV_WIDTH = 4
INNER = 4096
LANES = 128
VMEM_BYTES = 67043328
UP_CHUNKS = 4
TILE = 512

epsilon = 1e-06
F32 = jnp.float32
BF16 = jnp.bfloat16
MESH = pl.DeviceIdType.MESH


def product(left, right):
    return jnp.dot(left, right, preferred_element_type=F32)


def silu(x):
    return x * jax.nn.sigmoid(x)


def tiles(width):
    step = min(TILE, width)
    return [(start, step) for start in range(0, width, step)]


def lane_sum(x):
    return jnp.broadcast_to(jnp.sum(x, axis=1, keepdims=True), (x.shape[0], LANES))


def kernel(
    kv_count,
    tp_count,
    h_tokens,
    h_lengths,
    h_conv_state_x,
    h_conv_state_bc,
    h_norm_gain,
    h_mlp_gain,
    h_inner_gain,
    h_step_bias,
    h_decay_log,
    h_conv_x,
    h_conv_bc,
    ssm_state,
    w_gate,
    w_value,
    w_key,
    w_query,
    w_step,
    w_out,
    w_up,
    w_down,
    layer_out,
    next_state,
    v_gate,
    v_value,
    v_key,
    v_query,
    v_step,
    v_out,
    v_up,
    v_down,
    v_state,
    state_high,
    state_low,
    tokens,
    lengths,
    conv_state_x,
    conv_state_bc,
    norm_gain,
    mlp_gain,
    inner_gain,
    step_bias,
    decay_log,
    conv_x,
    conv_bc,
    mix_send,
    mix_recv,
    gate_send,
    gate_recv,
    step_send,
    step_recv,
    low_all,
    low_squares,
    out_all,
    out_squares,
    up_send,
    up_recv,
    up_sq_send,
    up_sq_recv,
    act_all,
    down_all,
    load_sems,
    kv_send_sems,
    kv_recv_sems,
    tp_send_sems,
    tp_recv_sems,
):
    z = lax.axis_index("kv")
    t = lax.axis_index("tp")
    rows = tokens.shape[0]
    seqs = rows // kv_count
    inner = v_value.shape[1]
    narrow = v_key.shape[1]
    heads = v_step.shape[0]
    group_count = narrow // STATE
    per_group = heads // group_count
    group_width = per_group * HEAD_DIM
    hidden = v_up.shape[1]
    chunk = hidden // UP_CHUNKS

    loads = {}

    def load(name, src, dst):
        copy = pltpu.make_async_copy(src, dst, load_sems.at[len(loads)])
        copy.start()
        loads[name] = copy

    load("tokens", h_tokens, tokens)
    load("norm_gain", h_norm_gain, norm_gain)
    load("value", w_value, v_value)
    load("key", w_key, v_key)
    load("query", w_query, v_query)
    load("step", w_step, v_step)
    load("gate", w_gate, v_gate)
    small = [
        ("lengths", h_lengths, lengths),
        ("conv_state_x", h_conv_state_x, conv_state_x),
        ("conv_state_bc", h_conv_state_bc, conv_state_bc),
        ("mlp_gain", h_mlp_gain, mlp_gain),
        ("inner_gain", h_inner_gain, inner_gain),
        ("step_bias", h_step_bias, step_bias),
        ("decay_log", h_decay_log, decay_log),
        ("conv_x", h_conv_x, conv_x),
        ("conv_bc", h_conv_bc, conv_bc),
    ]
    for item in small:
        load(*item)
    load("state", ssm_state, v_state)
    load("out", w_out, v_out)

    barrier = pltpu.get_barrier_semaphore()
    for d in range(1, kv_count):
        pl.semaphore_signal(
            barrier, inc=1, device_id={"kv": lax.rem(z + d, kv_count)}, device_id_type=MESH
        )
    for d in range(1, tp_count):
        pl.semaphore_signal(
            barrier, inc=1, device_id={"tp": lax.rem(t + d, tp_count)}, device_id_type=MESH
        )

    started = []

    def exchange(axis, stage, source, target):
        me, count, send_sems, recv_sems = (
            (z, kv_count, kv_send_sems, kv_recv_sems)
            if axis == "kv"
            else (t, tp_count, tp_send_sems, tp_recv_sems)
        )
        copies = []
        for d in range(1, count):
            peer = lax.rem(me + d, count)
            copy = pltpu.make_async_remote_copy(
                src_ref=source(peer),
                dst_ref=target(me),
                send_sem=send_sems.at[stage, d - 1],
                recv_sem=recv_sems.at[stage, d - 1],
                device_id={axis: peer},
                device_id_type=MESH,
            )
            copy.start()
            copies.append(copy)
        started.extend(copies)
        return copies

    def arrive(copies):
        for copy in copies:
            copy.wait_recv()

    def scatter_rows(ref, value, lead=()):
        for j in range(kv_count):
            ref[lead + (j,)] = value[j * seqs : (j + 1) * seqs].astype(ref.dtype)

    def total(ref, count, lead=()):
        acc = ref[lead + (0,)].astype(F32)
        for j in range(1, count):
            acc = acc + ref[lead + (j,)].astype(F32)
        return acc

    def gather_rows(ref, lead=()):
        return jnp.concatenate(
            [ref[lead + (j,)].astype(F32) for j in range(kv_count)], axis=0
        )

    def gain(ref):
        return ref[...].astype(F32).reshape(1, ref.shape[0])

    loads["tokens"].wait()
    loads["norm_gain"].wait()
    widened = tokens[...].astype(F32)
    scaled = (widened * gain(norm_gain)).astype(BF16)
    token_squares = lane_sum(widened * widened)

    def project(weights, send, offset):
        for start, size in tiles(weights.shape[1]):
            piece = product(scaled, weights[:, start : start + size])
            for j in range(kv_count):
                send[j, :, offset + start : offset + start + size] = piece[
                    j * seqs : (j + 1) * seqs
                ].astype(BF16)

    loads["value"].wait()
    project(v_value, mix_send, 0)
    loads["key"].wait()
    project(v_key, mix_send, inner)
    loads["query"].wait()
    project(v_query, mix_send, inner + narrow)
    loads["step"].wait()
    step_part = lax.dot_general(
        scaled, v_step[...], (((1,), (1,)), ((), ())), preferred_element_type=F32
    )
    step_part = jnp.concatenate(
        [step_part, jnp.zeros((rows, LANES - heads), F32), token_squares], axis=1
    )
    scatter_rows(step_send, step_part)
    pl.semaphore_wait(barrier, kv_count + tp_count - 2)
    step_copies = exchange("kv", 0, lambda p: step_send.at[p], lambda m: step_recv.at[m])
    mix_copies = exchange("kv", 1, lambda p: mix_send.at[p], lambda m: mix_recv.at[m])
    loads["gate"].wait()
    for c in range(UP_CHUNKS):
        load(
            f"up{c}",
            w_up.at[:, c * chunk : (c + 1) * chunk],
            v_up.at[:, c * chunk : (c + 1) * chunk],
        )
    for c in range(UP_CHUNKS):
        load(
            f"down{c}",
            w_down.at[c * chunk : (c + 1) * chunk],
            v_down.at[c * chunk : (c + 1) * chunk],
        )
    project(v_gate, gate_send, 0)
    gate_copies = exchange("kv", 2, lambda p: gate_send.at[p], lambda m: gate_recv.at[m])
    step_recv[z] = step_send[z]
    mix_recv[z] = mix_send[z]
    gate_recv[z] = gate_send[z]

    loads["state"].wait()
    for b in range(seqs):
        state = v_state[b]
        high = state.astype(BF16)
        state_high[b] = high
        state_low[b] = (state - high.astype(F32)).astype(BF16)

    for name, _, _ in small:
        loads[name].wait()
    seq_of = lax.broadcasted_iota(jnp.int32, (seqs, 1), 0)
    seen = jnp.zeros((seqs, 1), jnp.int32)
    for b in range(seqs):
        seen = jnp.where(seq_of == b, lengths[b], seen)
    lane_of = lax.broadcasted_iota(jnp.int32, (1, LANES), 1)
    bias_row = jnp.zeros((1, LANES), F32)
    log_row = jnp.zeros((1, LANES), F32)
    for h in range(heads):
        bias_row = jnp.where(lane_of == h, step_bias[h], bias_row)
        log_row = jnp.where(lane_of == h, decay_log[h], log_row)

    taps = jnp.concatenate(
        [conv_x[...].astype(F32)] + [conv_bc[:, i].astype(F32) for i in range(2)], axis=1
    )
    conv_old = jnp.zeros((seqs, inner + 2 * narrow), F32)
    for k in range(CONV_WIDTH - 1):
        held = jnp.concatenate(
            [conv_state_x[k].astype(F32)]
            + [conv_state_bc[:, k, i].astype(F32) for i in range(2)],
            axis=1,
        )
        live = jnp.where(seen >= CONV_WIDTH - 1 - k, 1.0, 0.0)
        conv_old = conv_old + held * live * taps[k : k + 1]
    conv_tap = taps[CONV_WIDTH - 1 :]

    arrive(step_copies)
    steps = total(step_recv, kv_count)
    inverse = lax.rsqrt(steps[:, LANES : LANES + 1] / D + epsilon)
    step_size = jax.nn.softplus(steps[:, :LANES] * inverse + bias_row)
    decay = jnp.exp(-jnp.exp(log_row) * step_size)
    head_of = lax.broadcasted_iota(jnp.int32, (LANES, inner), 1) // HEAD_DIM
    one_hot = jnp.where(
        head_of == lax.broadcasted_iota(jnp.int32, (LANES, inner), 0), 1.0, 0.0
    ).astype(F32)
    spread = jnp.dot(
        jnp.concatenate([step_size, decay], axis=0),
        one_hot,
        precision=lax.Precision.HIGHEST,
        preferred_element_type=F32,
    )
    step_wide, decay_wide = spread[:seqs], spread[seqs:]
    arrive(mix_copies)
    mixed = silu(conv_old + total(mix_recv, kv_count) * inverse * conv_tap)
    input_wide = step_wide * mixed[:, :inner]
    keys = mixed[:, inner : inner + narrow]
    queries = mixed[:, inner + narrow :]

    pieces = []
    for g in range(group_count):
        query = queries[:, g * STATE : (g + 1) * STATE]
        key = keys[:, g * STATE : (g + 1) * STATE]
        query_high = query.astype(BF16).astype(F32)
        both = jnp.concatenate([query_high, query - query_high], axis=0).astype(BF16)
        lines = []
        for b in range(seqs):
            span = slice(g * per_group, (g + 1) * per_group)
            high = state_high[b, span].reshape(group_width, STATE)
            low = state_low[b, span].reshape(group_width, STATE)
            dims = (((1,), (1,)), ((), ()))
            with_high = lax.dot_general(both, high, dims, preferred_element_type=F32)
            with_low = lax.dot_general(both, low, dims, preferred_element_type=F32)
            lines.append(
                with_high[b : b + 1] + with_high[seqs + b : seqs + b + 1] + with_low[b : b + 1]
            )
        from_state = jnp.concatenate(lines, axis=0)
        overlap = jnp.sum(key * query, axis=1, keepdims=True)
        columns = slice(g * group_width, (g + 1) * group_width)
        pieces.append(decay_wide[:, columns] * from_state + input_wide[:, columns] * overlap)
    mixer_y = jnp.concatenate(pieces, axis=1)
    arrive(gate_copies)
    gated = mixer_y * silu(total(gate_recv, kv_count) * inverse)
    low_all[z] = (gated * gain(inner_gain)).astype(BF16)
    low_squares[z] = lane_sum(gated * gated)
    low_copies = exchange("kv", 3, lambda p: low_all.at[z], lambda m: low_all.at[m])
    sq_copies = exchange("kv", 4, lambda p: low_squares.at[z], lambda m: low_squares.at[m])

    padded = jnp.concatenate(
        [input_wide, jnp.zeros((LANES - seqs, inner), F32)], axis=0
    )
    upright = jnp.transpose(padded)
    def update(first, last):
        for b in range(seqs * first // 4, seqs * last // 4):
            for h in range(heads):
                g = h // per_group
                next_state[b, h] = (
                    v_state[b, h] * decay[b : b + 1, h : h + 1]
                    + upright[h * HEAD_DIM : (h + 1) * HEAD_DIM, b : b + 1]
                    * keys[b : b + 1, g * STATE : (g + 1) * STATE]
                )

    update(0, 1)

    loads["out"].wait()
    arrive(low_copies)
    lows = gather_rows(low_all).astype(BF16)
    for start, size in tiles(v_out.shape[1]):
        out_all[t, :, start : start + size] = product(
            lows, v_out[:, start : start + size]
        ).astype(BF16)
    arrive(sq_copies)
    out_squares[t] = gather_rows(low_squares)
    out_copies = exchange("tp", 0, lambda p: out_all.at[t], lambda m: out_all.at[m])
    out_sq_copies = exchange("tp", 1, lambda p: out_squares.at[t], lambda m: out_squares.at[m])
    update(1, 2)
    arrive(out_sq_copies)
    out_inverse = lax.rsqrt(total(out_squares, tp_count)[:, :1] / INNER + epsilon)
    arrive(out_copies)
    residual = (widened + total(out_all, tp_count) * out_inverse).astype(BF16).astype(F32)
    hidden_low = (residual * gain(mlp_gain)).astype(BF16)
    scatter_rows(up_sq_send, lane_sum(residual * residual))
    up_sq_copies = exchange("kv", 5, lambda p: up_sq_send.at[p], lambda m: up_sq_recv.at[m])

    up_copies = []
    for c in range(UP_CHUNKS):
        loads[f"up{c}"].wait()
        for start, size in tiles(chunk):
            base = c * chunk + start
            piece = product(hidden_low, v_up[:, base : base + size])
            for j in range(kv_count):
                up_send[c, j, :, start : start + size] = piece[
                    j * seqs : (j + 1) * seqs
                ].astype(BF16)
        up_copies.append(
            exchange(
                "kv",
                6 + c,
                lambda p, c=c: up_send.at[c, p],
                lambda m, c=c: up_recv.at[c, m],
            )
        )
        up_recv[c, z] = up_send[c, z]
    up_sq_recv[z] = up_sq_send[z]
    update(2, 3)
    arrive(up_sq_copies)
    up_inverse = lax.rsqrt(total(up_sq_recv, kv_count)[:, :1] / D + epsilon)
    act_copies = []
    for c in range(UP_CHUNKS):
        arrive(up_copies[c])
        active = jnp.maximum(total(up_recv, kv_count, (c,)) * up_inverse, 0.0)
        act_all[c, z] = (active * active).astype(BF16)
        act_copies.append(
            exchange(
                "kv",
                6 + UP_CHUNKS + c,
                lambda p, c=c: act_all.at[c, z],
                lambda m, c=c: act_all.at[c, m],
            )
        )
    down = jnp.zeros((rows, v_down.shape[1]), F32)
    for c in range(UP_CHUNKS):
        loads[f"down{c}"].wait()
        arrive(act_copies[c])
        acts = gather_rows(act_all, (c,)).astype(BF16)
        down = down + product(acts, v_down[c * chunk : (c + 1) * chunk])
    down_all[t] = down.astype(BF16)
    down_copies = exchange("tp", 2, lambda p: down_all.at[t], lambda m: down_all.at[m])
    update(3, 4)
    arrive(down_copies)
    layer_out[...] = (residual + total(down_all, tp_count)).astype(BF16)
    for copy in started:
        copy.wait_send()


def per_device(
    kv_count,
    tp_count,
    tokens,
    lengths,
    conv_state_x,
    conv_state_bc,
    ssm_state,
    norm_gain,
    w_gate,
    w_value,
    w_key,
    w_query,
    w_step,
    step_bias,
    decay_log,
    conv_x,
    conv_bc,
    inner_gain,
    w_out,
    mlp_gain,
    w_up,
    w_down,
):
    rows, depth = tokens.shape
    seqs = lengths.shape[0]
    inner, narrow, heads = w_value.shape[1], w_key.shape[1], w_step.shape[1]
    hidden = w_up.shape[1]
    chunk = hidden // UP_CHUNKS
    results = 4 * ssm_state.size + 2 * rows * w_out.shape[1]
    grant = (VMEM_BYTES - results) // 4096 * 4096 - 4096
    vmem = pl.BlockSpec(memory_space=pltpu.VMEM)
    hbm = pl.BlockSpec(memory_space=pltpu.HBM)
    mixed = inner + 2 * narrow
    width = w_out.shape[1]
    stages = 6 + 2 * UP_CHUNKS
    return pl.pallas_call(
        functools.partial(kernel, kv_count, tp_count),
        out_shape=(
            pltpu.VMEM((rows, width), BF16),
            pltpu.VMEM(ssm_state.shape, F32),
        ),
        in_specs=[hbm] * 20,
        out_specs=(vmem, vmem),
        scratch_shapes=[
            pltpu.VMEM(w_gate.shape, BF16),
            pltpu.VMEM(w_value.shape, BF16),
            pltpu.VMEM(w_key.shape, BF16),
            pltpu.VMEM(w_query.shape, BF16),
            pltpu.VMEM(w_step.shape[::-1], BF16),
            pltpu.VMEM(w_out.shape, BF16),
            pltpu.VMEM(w_up.shape, BF16),
            pltpu.VMEM(w_down.shape, BF16),
            pltpu.VMEM(ssm_state.shape, F32),
            pltpu.VMEM(ssm_state.shape, BF16),
            pltpu.VMEM(ssm_state.shape, BF16),
            pltpu.VMEM(tokens.shape, BF16),
            pltpu.SMEM(lengths.shape, jnp.int32),
            pltpu.VMEM((CONV_WIDTH - 1, seqs, inner), BF16),
            pltpu.VMEM(conv_state_bc.shape, BF16),
            pltpu.VMEM(norm_gain.shape, BF16),
            pltpu.VMEM(mlp_gain.shape, BF16),
            pltpu.VMEM(inner_gain.shape, BF16),
            pltpu.SMEM(step_bias.shape, F32),
            pltpu.SMEM(decay_log.shape, F32),
            pltpu.VMEM(conv_x.shape, BF16),
            pltpu.VMEM(conv_bc.shape, BF16),
            pltpu.VMEM((kv_count, seqs, mixed), BF16),
            pltpu.VMEM((kv_count, seqs, mixed), BF16),
            pltpu.VMEM((kv_count, seqs, inner), BF16),
            pltpu.VMEM((kv_count, seqs, inner), BF16),
            pltpu.VMEM((kv_count, seqs, 2 * LANES), F32),
            pltpu.VMEM((kv_count, seqs, 2 * LANES), F32),
            pltpu.VMEM((kv_count, seqs, inner), BF16),
            pltpu.VMEM((kv_count, seqs, LANES), F32),
            pltpu.VMEM((tp_count, rows, width), BF16),
            pltpu.VMEM((tp_count, rows, LANES), F32),
            pltpu.VMEM((UP_CHUNKS, kv_count, seqs, chunk), BF16),
            pltpu.VMEM((UP_CHUNKS, kv_count, seqs, chunk), BF16),
            pltpu.VMEM((kv_count, seqs, LANES), F32),
            pltpu.VMEM((kv_count, seqs, LANES), F32),
            pltpu.VMEM((UP_CHUNKS, kv_count, seqs, chunk), BF16),
            pltpu.VMEM((tp_count, rows, width), BF16),
            pltpu.SemaphoreType.DMA((18 + 2 * UP_CHUNKS,)),
            pltpu.SemaphoreType.DMA((stages, max(kv_count - 1, 1))),
            pltpu.SemaphoreType.DMA((stages, max(kv_count - 1, 1))),
            pltpu.SemaphoreType.DMA((3, max(tp_count - 1, 1))),
            pltpu.SemaphoreType.DMA((3, max(tp_count - 1, 1))),
        ],
        compiler_params=pltpu.CompilerParams(
            collective_id=0, has_side_effects=True, vmem_limit_bytes=grant
        ),
    )(
        tokens,
        lengths,
        jnp.swapaxes(conv_state_x, 0, 1),
        conv_state_bc,
        norm_gain,
        mlp_gain,
        inner_gain,
        step_bias,
        decay_log,
        conv_x,
        conv_bc,
        ssm_state,
        w_gate,
        w_value,
        w_key,
        w_query,
        w_step.T,
        w_out,
        w_up,
        w_down,
    )


def solution(mesh):
    return jax.shard_map(
        functools.partial(per_device, mesh.shape["kv"], mesh.shape["tp"]),
        mesh=mesh,
        in_specs=(
            P("grp", "kv"),
            P(("grp", "kv")),
            P(("grp", "kv"), None, "tp"),
            P(("grp", "kv"), None, None, "tp"),
            P(("grp", "kv"), "tp", None, None),
            P("kv"),
            P("kv", "tp"),
            P("kv", "tp"),
            P("kv", "tp"),
            P("kv", "tp"),
            P("kv", "tp"),
            P("tp"),
            P("tp"),
            P(None, "tp"),
            P(None, None, "tp"),
            P("tp"),
            P("tp", "kv"),
            P("kv"),
            P("kv", "tp"),
            P("tp", "kv"),
        ),
        out_specs=(P("grp", "kv"), P(("grp", "kv"), "tp", None, None)),
        check_vma=False,
    )
```
